32 devices in a mesh: ep: 16 (over z, y, x), tp: 2 (over core).
Axes of the slice: x: 2, y: 2, z: 4, core: 2. Of those that a mesh axis runs over, the one named last changes fastest.
Arguments:
- tokens: bfloat16 [8192, 2048], P(('ep', 'tp')), may hold values from -6 to 6
- norm_gain: float32 [2048], replicated, may hold values from 0.1 to 1.9
- expert_ids: int32 [8192, 2], P(('ep', 'tp')), may hold values from 0 to 15, all different within a row; in each aligned block of 256 rows (0 to 255, 256 to 511, ...) at most 48 rows name the same one
- route_weights: float32 [8192, 2], P(('ep', 'tp')), may hold values from 0.2 to 1.2
- expert_gate: bfloat16 [16, 2048, 512], P('ep', None, 'tp'), may hold values from -0.125 to 0.125
- expert_up: bfloat16 [16, 2048, 512], P('ep', None, 'tp'), may hold values from -0.125 to 0.125
- expert_down: bfloat16 [16, 512, 2048], P('ep', 'tp'), may hold values from -0.25 to 0.25
- shared_gate: bfloat16 [2048, 512], P(None, 'tp'), may hold values from -0.125 to 0.125
- shared_up: bfloat16 [2048, 512], P(None, 'tp'), may hold values from -0.125 to 0.125
- shared_down: bfloat16 [512, 2048], P('tp'), may hold values from -0.25 to 0.25
Outputs:
- mixed: bfloat16 [8192, 2048], P(('ep', 'tp'))
The draws below stay inside these ranges and needn't reach their ends.
Inputs may be any that keep to these rules, and one draw needn't show every extreme that they name: `expert_ids`: each token names 2 different experts. Among the tokens of one device (aligned blocks of 256 rows) no expert is named by more than 48 tokens, and in every block some expert is named by exactly 48.
All inputs are finite; a program needn't handle non-finite values.
Results may differ from the reference program's by a relative error of at most 0.0075.
Values may be sent and summed in bfloat16 or wider, within the bound.
A program may use at most 64 MiB of HBM per device.

```python
import math
import jax
import jax.numpy as jnp
import numpy as np
from jax import lax

D = 2048
DE = 512
DS = 512
TOP_K = 2
TOK_DEV = 256
EXPERTS = 16
CAP = 48
TOKENS = 8192
N_EP = 16
N_TP = 2


def block_scale(key, shape, pieces, smallest, top_value):
    factor_of, own = 1.0, jax.random.fold_in(key, 6)
    for axis_at, blocks in pieces:
        draws = jnp.exp(jax.random.uniform(jax.random.fold_in(own, axis_at), (blocks,), jnp.float32, smallest / len(pieces), top_value / len(pieces)))
        factor_of = factor_of * jnp.repeat(draws, shape[axis_at] // blocks).reshape([-1 if axis == axis_at else 1 for axis in range(len(shape))])
    return factor_of


def assign_block(key, own, number, rows, amount, top, most, skew):
    order = jax.random.permutation(key, amount)
    heavy_load, ordinary = load_shares(amount, rows * top, most, skew, True), load_shares(amount, rows * top, most, skew, False)
    places = jnp.arange(amount)

    def named(lengths, offset_by):
        used = int((lengths > 0).sum())
        fixed = max(1, used // 4)
        moved = fixed + (places - fixed + offset_by * (used - fixed)) % max(1, amount - fixed)
        return jnp.zeros((amount,), jnp.int32).at[order[jnp.where(places < fixed, places, moved)]].set(jnp.asarray(lengths, jnp.int32))

    lengths = jnp.where(number % 4 == 0, named(heavy_load, number // 4), named(ordinary, number - number // 4 - 1))
    mixed = jax.random.permutation(jax.random.fold_in(own, 3), amount)
    giver, sink = mixed[0:amount // 2 * 2:2], mixed[1:amount // 2 * 2:2]
    slack = jnp.minimum(lengths[giver] - 1, most - lengths[sink]) // 2
    slack = jnp.where((giver == order[0]) | (sink == order[0]) | (lengths[sink] == 0), 0, jnp.maximum(slack, 0))
    moved = jax.random.randint(jax.random.fold_in(own, 4), (amount // 2,), 0, 1 << 20) % (slack + 1)
    lengths = lengths.at[giver].add(-moved).at[sink].add(moved)
    items = jnp.searchsorted(jnp.cumsum(lengths), jnp.arange(rows * top), side="right").astype(jnp.int32)
    grid = items.reshape(top, rows).T
    grid = grid[jax.random.permutation(jax.random.fold_in(own, 1), rows)]
    offset_by = jax.random.randint(jax.random.fold_in(own, 2), (rows, 1), 0, top)
    return jnp.take_along_axis(grid, (jnp.arange(top)[None, :] + offset_by) % top, axis=1)


def load_shares(number_of, total, limit, skew, full):
    portions = [(1 << 20) // math.isqrt(standing ** skew) + 1 for standing in range(1, number_of + 1)]
    largest = limit if full else min(limit, max(-(-total // number_of), total * portions[0] // sum(portions)))
    least = 1 if total - largest >= number_of - 1 else 0
    holding, spare = [largest] + [least] * (number_of - 1), total - largest - least * (number_of - 1)
    while spare > 0:
        movable = [i for i in range(1, number_of) if holding[i] < largest] or [i for i in range(1, number_of) if holding[i] < limit]
        mass, left = sum([portions[i] for i in movable]), spare
        for i in movable:
            addition = min(limit - holding[i], max(1, left * portions[i] // mass), spare)
            holding[i] = holding[i] + addition
            spare = spare - addition
    return np.array(holding)


def noise(own_key, extent, spread, reach, split=(), kind=jnp.bfloat16):
    gain = block_scale(own_key, extent, split, -0.22, 0.18) if split else 1.0
    array = jax.random.normal(own_key, extent, jnp.float32) * spread * gain
    return jnp.minimum(jnp.maximum(array, -reach), reach).astype(kind)


def setup_inputs(seed: int = 0) -> dict:
    key_of = jax.random.split(jax.random.key(seed), 11)
    tokens = noise(key_of[0], (TOKENS, D), 1.0, 6.0, ((0, 32),))
    norm_gain = jnp.clip(1.0 + 0.18 * jax.random.normal(key_of[1], (D,), jnp.float32), 0.1, 1.9)
    expert_ids_keys = jax.random.split(jax.random.fold_in(key_of[2], 1), TOKENS // TOK_DEV)
    expert_ids_turns = jax.random.permutation(jax.random.fold_in(key_of[2], 3), TOKENS // TOK_DEV)
    expert_ids = jax.vmap(lambda own, number: assign_block(jax.random.fold_in(key_of[2], 2), own, number, TOK_DEV, EXPERTS, TOP_K, CAP, 2))(expert_ids_keys, expert_ids_turns).reshape((TOKENS, TOP_K))
    route_weights = jnp.clip(0.2 + 1 * jax.random.uniform(key_of[3], (TOKENS, TOP_K), jnp.float32) ** block_scale(key_of[3], (TOKENS, TOP_K), ((0, 32),), -0.2, 0.2), 0.2, 1.2)
    expert_gate = noise(key_of[4], (EXPERTS, D, DE), D ** -0.5, 0.125, ((0, 16), (2, 2)))
    expert_up = noise(key_of[5], (EXPERTS, D, DE), D ** -0.5, 0.125, ((0, 16), (2, 2)))
    expert_down = noise(key_of[6], (EXPERTS, DE, D), DE ** -0.5, 0.25, ((0, 16), (1, 2)))
    shared_gate = noise(key_of[7], (D, DS), D ** -0.5, 0.125, ((1, 2),))
    shared_up = noise(key_of[8], (D, DS), D ** -0.5, 0.125, ((1, 2),))
    shared_down = noise(key_of[9], (DS, D), DS ** -0.5, 0.25, ((0, 2),))
    return {"tokens": tokens, "norm_gain": norm_gain, "expert_ids": expert_ids, "route_weights": route_weights, "expert_gate": expert_gate, "expert_up": expert_up, "expert_down": expert_down, "shared_gate": shared_gate, "shared_up": shared_up, "shared_down": shared_down}


epsilon = 1e-06

def normalize(tokens, norm_gain):
    values = tokens.astype(jnp.float32)
    factor = lax.rsqrt(lax.optimization_barrier(jnp.mean(values * values, axis=1, keepdims=True)) + epsilon)
    return (values * factor * norm_gain[None, :]).astype(jnp.bfloat16)

def halves(row_block, gate_w, up_w, down_w):
    half_width = gate_w.shape[1] // N_TP
    summed = jnp.zeros((row_block.shape[0], down_w.shape[1]), jnp.float32)
    for portion in range(N_TP):
        first = portion * half_width
        gate_value = jnp.dot(row_block, gate_w[:, first:first + half_width], preferred_element_type=jnp.float32)
        up_value = jnp.dot(row_block, up_w[:, first:first + half_width], preferred_element_type=jnp.float32)
        hidden = (jax.nn.silu(gate_value) * up_value).astype(jnp.bfloat16)
        partial_value = jnp.dot(hidden, down_w[first:first + half_width], preferred_element_type=jnp.float32)
        rounded = lax.optimization_barrier(partial_value.astype(jnp.bfloat16))
        summed = summed + rounded.astype(jnp.float32)
    return summed

def reference(tokens, norm_gain, expert_ids, route_weights, expert_gate, expert_up, expert_down, shared_gate, shared_up, shared_down):
    normed = normalize(tokens, norm_gain)
    total_rows = tokens.shape[0]
    shared_out = halves(normed, shared_gate, shared_up, shared_down)
    flat_ids = expert_ids.reshape(-1).astype(jnp.int32)
    assigned = flat_ids.shape[0]
    ordering = jnp.argsort(flat_ids, stable=True).astype(jnp.int32)
    counts = jnp.bincount(flat_ids, length=EXPERTS).astype(jnp.int32)
    starts = (jnp.cumsum(counts) - counts).astype(jnp.int32)
    most_rows = N_EP * N_TP * CAP
    padded = jnp.concatenate([normed, jnp.zeros((1, D), jnp.bfloat16)], axis=0)
    flat_weights = route_weights.reshape(-1)

    def per_expert(totals, expert):
        slot_range = jnp.arange(most_rows, dtype=jnp.int32)
        filled = slot_range < counts[expert]
        row_index = jnp.minimum(starts[expert] + slot_range, assigned - 1)
        assign = jnp.where(filled, ordering[row_index], assigned)
        token_index = (assign // TOP_K).astype(jnp.int32)
        row_block = padded[token_index]
        expert_out = halves(row_block, expert_gate[expert], expert_up[expert], expert_down[expert]).astype(jnp.bfloat16)
        weight_rows = jnp.where(filled, flat_weights[jnp.minimum(assign, assigned - 1)], jnp.float32(0.0))
        totals = totals.at[token_index].add(expert_out.astype(jnp.float32) * weight_rows[:, None])
        return (totals, None)
    totals, _ = lax.scan(per_expert, jnp.zeros((total_rows + 1, D), jnp.float32), jnp.arange(EXPERTS, dtype=jnp.int32))
    routed = totals[:total_rows]
    return (routed + shared_out).astype(jnp.bfloat16)
```

```python
import functools

import jax
import jax.numpy as jnp
from jax import lax
from jax.experimental import pallas as pl
from jax.experimental.pallas import tpu as pltpu
from jax.sharding import PartitionSpec as P

epsilon = 1e-06
MESH = pl.DeviceIdType.MESH


def toggled(index, step, size):
    total, bit = 0, 1
    while bit < size:
        total = total + bit * ((index // bit + step // bit) % 2)
        bit *= 2
    return total


def gated_sum(rows, gate_w, up_w, down_w):
    total = None
    for half in range(gate_w.shape[0]):
        gate_value = jnp.dot(rows, gate_w[half], preferred_element_type=jnp.float32)
        up_value = jnp.dot(rows, up_w[half], preferred_element_type=jnp.float32)
        hidden = (gate_value / (1.0 + jnp.exp(-gate_value)) * up_value).astype(jnp.bfloat16)
        term = jnp.dot(hidden, down_w[half], preferred_element_type=jnp.float32)
        total = term if total is None else total + term
    return total


def layer_kernel(
    peers,
    capacity,
    tokens,
    gain,
    ids_row,
    ids_col,
    weights_col,
    expert_gate,
    expert_up,
    expert_down,
    shared_gate,
    shared_up,
    shared_down,
    mixed,
    gate_all,
    up_all,
    down_all,
    s_gate_all,
    s_up_all,
    s_down_all,
    normed,
    outgoing,
    received,
    results,
    returned,
    total,
    weight_local,
    weight_send,
    weight_recv,
    out_send,
    out_recv,
    back_send,
    back_recv,
):
    me = lax.axis_index("ep")
    core = lax.axis_index("tp")
    sibling = 1 - core
    tok_rows = tokens.shape[0]
    group = 4
    barrier = pltpu.get_barrier_semaphore()
    pl.semaphore_signal(barrier, inc=1, device_id=(me, sibling), device_id_type=MESH)
    for step in range(1, peers):
        pl.semaphore_signal(
            barrier, inc=1, device_id=(toggled(me, step, peers), core), device_id_type=MESH
        )
    sources = (
        (shared_gate, s_gate_all),
        (shared_up, s_up_all),
        (shared_down, s_down_all),
        (expert_gate, gate_all),
        (expert_up, up_all),
        (expert_down, down_all),
    )
    local = [
        pltpu.make_async_copy(source, target.at[core], weight_local.at[i])
        for i, (source, target) in enumerate(sources)
    ]
    for copy in local:
        copy.start()

    values = tokens[...].astype(jnp.float32)
    factor = lax.rsqrt(jnp.mean(values * values, axis=1, keepdims=True) + epsilon)
    normed[...] = (values * factor * gain[...]).astype(jnp.bfloat16)

    relative = ids_row[...] ^ me
    step_of = lax.broadcasted_iota(jnp.int32, (peers, tok_rows), 0)
    named = (step_of == relative[0:1, :]) | (step_of == relative[1:2, :])
    row_at = lax.broadcasted_iota(jnp.int32, (tok_rows, tok_rows), 0)
    col_at = lax.broadcasted_iota(jnp.int32, (tok_rows, tok_rows), 1)
    before = jnp.where(row_at < col_at, 1.0, 0.0).astype(jnp.bfloat16)
    slots = jnp.dot(
        jnp.where(named, 1.0, 0.0).astype(jnp.bfloat16), before, preferred_element_type=jnp.float32
    ).astype(jnp.int32)
    slots = jnp.where(named, slots, -1)
    slot_at = lax.broadcasted_iota(jnp.int32, (capacity, tok_rows), 0)

    def pick(step):
        return jnp.where(slot_at == slots[step : step + 1, :], 1.0, 0.0).astype(jnp.bfloat16)

    def dispatch(step):
        return pltpu.make_async_remote_copy(
            src_ref=outgoing.at[step],
            dst_ref=received.at[step],
            send_sem=out_send.at[step],
            recv_sem=out_recv.at[step],
            device_id=(toggled(me, step, peers), core),
            device_id_type=MESH,
        )

    def give_back(step):
        return pltpu.make_async_remote_copy(
            src_ref=results.at[step],
            dst_ref=returned.at[step],
            send_sem=back_send.at[step],
            recv_sem=back_recv.at[step],
            device_id=(toggled(me, step, peers), core),
            device_id_type=MESH,
        )

    started = False
    for first in range(peers - group, -1, -group):
        picked = jnp.concatenate([pick(first + i) for i in range(group)], axis=0)
        rows = jnp.dot(picked, normed[...], preferred_element_type=jnp.float32).astype(jnp.bfloat16)
        for i in range(group):
            block = rows[i * capacity : (i + 1) * capacity]
            if first + i == 0:
                received[0] = block
            else:
                outgoing[first + i] = block
        if not started:
            pl.semaphore_wait(barrier, peers)
            started = True
        for i in range(group):
            if first + i:
                dispatch(first + i).start()

    remote = [
        pltpu.make_async_remote_copy(
            src_ref=source,
            dst_ref=target.at[core],
            send_sem=weight_send.at[i],
            recv_sem=weight_recv.at[i],
            device_id=(me, sibling),
            device_id_type=MESH,
        )
        for i, (source, target) in enumerate(sources)
    ]
    for copy in remote:
        copy.start()
    for i in range(len(sources)):
        local[i].wait()
        remote[i].wait()

    def take(pair, carry):
        for i in range(2):
            step = 2 * pair + i

            @pl.when(step > 0)
            def _():
                dispatch(step).wait_recv()

        block = received[pl.ds(2 * pair, 2)].reshape(2 * capacity, received.shape[2])
        out = gated_sum(block, gate_all, up_all, down_all).astype(jnp.bfloat16)
        for i in range(2):
            step = 2 * pair + i
            part = out[i * capacity : (i + 1) * capacity]

            @pl.when(step > 0)
            def _():
                results[step] = part
                give_back(step).start()

            @pl.when(step == 0)
            def _():
                returned[step] = part

        return carry

    total[...] = gated_sum(normed[...], s_gate_all, s_up_all, s_down_all)
    lax.fori_loop(0, peers // 2, take, 0)

    relative_col = ids_col[...] ^ me
    expert_at = lax.broadcasted_iota(jnp.int32, (tok_rows, 128), 1)
    chosen = [expert_at == relative_col[:, j : j + 1] for j in range(2)]
    after = jnp.where(row_at > col_at, 1.0, 0.0).astype(jnp.bfloat16)
    counted = jnp.dot(
        after,
        jnp.where(chosen[0] | chosen[1], 1.0, 0.0).astype(jnp.bfloat16),
        preferred_element_type=jnp.float32,
    )
    places = [
        relative_col[:, j : j + 1] * capacity
        + jnp.sum(jnp.where(chosen[j], counted, 0.0), axis=1, keepdims=True).astype(jnp.int32)
        for j in range(2)
    ]
    for first in range(0, peers, group):
        for i in range(group):
            if first + i:
                give_back(first + i).wait_recv()
        at = lax.broadcasted_iota(jnp.int32, (tok_rows, group * capacity), 1) + first * capacity
        scale = jnp.where(at == places[0], weights_col[:, 0:1], 0.0) + jnp.where(
            at == places[1], weights_col[:, 1:2], 0.0
        )
        upper = scale.astype(jnp.bfloat16)
        lower = (scale - upper.astype(jnp.float32)).astype(jnp.bfloat16)
        block = returned[first : first + group].reshape(group * capacity, returned.shape[2])
        term = jnp.dot(upper, block, preferred_element_type=jnp.float32) + jnp.dot(
            lower, block, preferred_element_type=jnp.float32
        )
        if first + group < peers:
            total[...] += term
        else:
            mixed[...] = (total[...] + term).astype(jnp.bfloat16)
    for step in range(1, peers):
        dispatch(step).wait_send()
        give_back(step).wait_send()


def kernel_body(
    tokens,
    norm_gain,
    expert_ids,
    route_weights,
    expert_gate,
    expert_up,
    expert_down,
    shared_gate,
    shared_up,
    shared_down,
):
    peers = lax.axis_size("ep")
    halves = lax.axis_size("tp")
    tok_rows, width = tokens.shape
    capacity = 3 * tok_rows * expert_ids.shape[1] // (2 * peers)
    vmem = pl.BlockSpec(memory_space=pltpu.VMEM)
    anywhere = pl.BlockSpec(memory_space=pl.ANY)
    slots = pltpu.VMEM((peers, capacity, width), jnp.bfloat16)
    weights = (
        expert_gate[0],
        expert_up[0],
        expert_down[0],
        shared_gate,
        shared_up,
        shared_down,
    )
    dma = pltpu.SemaphoreType.DMA
    return pl.pallas_call(
        functools.partial(layer_kernel, peers, capacity),
        out_shape=jax.ShapeDtypeStruct((tok_rows, width), jnp.bfloat16),
        in_specs=[vmem] * 5 + [anywhere] * 6,
        out_specs=vmem,
        scratch_shapes=[pltpu.VMEM((halves,) + w.shape, w.dtype) for w in weights]
        + [pltpu.VMEM((tok_rows, width), jnp.bfloat16), slots, slots, slots, slots]
        + [pltpu.VMEM((tok_rows, width), jnp.float32)]
        + [dma((len(weights),))] * 3
        + [dma((peers,))] * 4,
        compiler_params=pltpu.CompilerParams(
            collective_id=0, has_side_effects=True, vmem_limit_bytes=56 * 1024 * 1024
        ),
        name="layer",
    )(
        tokens,
        norm_gain.reshape(1, width),
        expert_ids.T,
        expert_ids,
        route_weights,
        *weights,
    )


def normalize(tokens, norm_gain):
    values = tokens.astype(jnp.float32)
    factor = lax.rsqrt(jnp.mean(values * values, axis=1, keepdims=True) + epsilon)
    return (values * factor * norm_gain[None, :]).astype(jnp.bfloat16)


def round_term(partial_value):
    return lax.optimization_barrier(partial_value.astype(jnp.bfloat16)).astype(jnp.float32)


def gated_rows(row_block, gate_w, up_w):
    gate_value = jnp.dot(row_block, gate_w, preferred_element_type=jnp.float32)
    up_value = jnp.dot(row_block, up_w, preferred_element_type=jnp.float32)
    return (jax.nn.silu(gate_value) * up_value).astype(jnp.bfloat16)


def sliced_term(hidden, down_w):
    return round_term(jnp.dot(hidden, down_w, preferred_element_type=jnp.float32))


def shared_branch(normed, shared_gate, shared_up, shared_down):
    hidden = gated_rows(lax.all_gather(normed, "tp", axis=0, tiled=True), shared_gate, shared_up)
    return lax.psum_scatter(
        sliced_term(hidden, shared_down).astype(jnp.bfloat16), "tp", scatter_dimension=0, tiled=True
    ).astype(jnp.float32)


def body(
    tokens,
    norm_gain,
    expert_ids,
    route_weights,
    expert_gate,
    expert_up,
    expert_down,
    shared_gate,
    shared_up,
    shared_down,
):
    normed = normalize(tokens, norm_gain)
    tok_rows = tokens.shape[0]
    model_width = tokens.shape[1]
    top_count = expert_ids.shape[1]
    ep_size = lax.axis_size("ep")
    experts = expert_gate.shape[0] * ep_size
    capacity = 3 * tok_rows * top_count // (2 * experts)
    assigned = tok_rows * top_count
    gate_one = expert_gate[0]
    up_one = expert_up[0]
    down_one = expert_down[0]
    flat_ids = expert_ids.reshape(-1)
    onehot = (flat_ids[:, None] == jnp.arange(experts, dtype=jnp.int32)[None, :]).astype(
        jnp.bfloat16
    )
    earlier = (jnp.arange(assigned)[:, None] > jnp.arange(assigned)[None, :]).astype(jnp.bfloat16)
    before_count = jnp.dot(earlier, onehot, preferred_element_type=jnp.float32)
    slot_index = jnp.sum(before_count * onehot.astype(jnp.float32), axis=1).astype(jnp.int32)
    position = flat_ids * capacity + slot_index
    owners = (
        jnp.full((experts * capacity,), tok_rows, jnp.int32)
        .at[position]
        .set(jnp.arange(assigned, dtype=jnp.int32) // top_count)
    )
    padded = jnp.concatenate([normed, jnp.zeros((1, model_width), jnp.bfloat16)], axis=0)
    outgoing = padded[owners].reshape(ep_size, capacity, model_width)
    half_slots = capacity // 2
    split_rows = outgoing.reshape(ep_size, 2, half_slots, model_width)
    results = []
    for portion in range(2):
        received = lax.all_to_all(
            split_rows[:, portion], "ep", split_axis=0, concat_axis=0, tiled=True
        )
        hidden = gated_rows(
            lax.all_gather(
                received.reshape(ep_size * half_slots, model_width), "tp", axis=0, tiled=True
            ),
            gate_one,
            up_one,
        )
        summed = lax.psum_scatter(
            sliced_term(hidden, down_one).astype(jnp.bfloat16),
            "tp",
            scatter_dimension=0,
            tiled=True,
        )
        results.append(
            lax.all_to_all(
                summed.reshape(ep_size, half_slots, model_width),
                "ep",
                split_axis=0,
                concat_axis=0,
                tiled=True,
            )
        )
    returned = jnp.stack(results, axis=1)
    gathered = returned.reshape(experts * capacity, model_width)[position]
    routed = jnp.sum(
        gathered.reshape(tok_rows, top_count, model_width).astype(jnp.float32)
        * route_weights[:, :, None],
        axis=1,
    )
    shared_out = shared_branch(normed, shared_gate, shared_up, shared_down)
    return (routed + shared_out).astype(jnp.bfloat16)


def plan_of(*args):
    peers = lax.axis_size("ep")
    capacity = 3 * args[0].shape[0] * args[2].shape[1] // (2 * peers)
    whole_tiles = capacity % 16 == 0 and peers % 4 == 0 and peers & (peers - 1) == 0
    fits = whole_tiles and lax.axis_size("tp") == 2 and args[4].shape[0] == 1
    return (kernel_body if fits else body)(*args)


def solution(mesh):
    placed = (
        P(("ep", "tp"), None),
        P(),
        P(("ep", "tp"), None),
        P(("ep", "tp"), None),
        P("ep", None, "tp"),
        P("ep", None, "tp"),
        P("ep", "tp", None),
        P(None, "tp"),
        P(None, "tp"),
        P("tp", None),
    )
    return jax.shard_map(
        plan_of, mesh=mesh, in_specs=placed, out_specs=P(("ep", "tp"), None), check_vma=False
    )
```

```python
import functools

import jax
import jax.numpy as jnp
from jax import lax
from jax.experimental import pallas as pl
from jax.experimental.pallas import tpu as pltpu
from jax.sharding import PartitionSpec as P

epsilon = 1e-06
MESH = pl.DeviceIdType.MESH


def toggled(index, step, size):
    total, bit = 0, 1
    while bit < size:
        total = total + bit * ((index // bit + step // bit) % 2)
        bit *= 2
    return total


def gated_sum(rows, gate_w, up_w, down_w):
    total = None
    for half in range(gate_w.shape[0]):
        gate_value = jnp.dot(rows, gate_w[half], preferred_element_type=jnp.float32)
        up_value = jnp.dot(rows, up_w[half], preferred_element_type=jnp.float32)
        hidden = (gate_value / (1.0 + jnp.exp(-gate_value)) * up_value).astype(jnp.bfloat16)
        term = jnp.dot(hidden, down_w[half], preferred_element_type=jnp.float32)
        total = term if total is None else total + term
    return total


def slot_rows(meta, me, steps):
    count = meta.shape[1]
    relative = meta[0:2, :].astype(jnp.int32) ^ me
    step_of = lax.broadcasted_iota(jnp.int32, (steps, count), 0)
    named = (step_of == relative[0:1, :]) | (step_of == relative[1:2, :])
    row_at = lax.broadcasted_iota(jnp.int32, (count, count), 0)
    col_at = lax.broadcasted_iota(jnp.int32, (count, count), 1)
    before = jnp.where(row_at < col_at, 1.0, 0.0).astype(jnp.bfloat16)
    slots = jnp.dot(
        jnp.where(named, 1.0, 0.0).astype(jnp.bfloat16), before, preferred_element_type=jnp.float32
    ).astype(jnp.int32)
    return jnp.where(named, slots, -1)


def picks(slots, steps, capacity):
    slot_at = lax.broadcasted_iota(jnp.int32, (capacity, slots.shape[1]), 0)
    return jnp.concatenate(
        [
            jnp.where(slot_at == slots[step : step + 1, :], 1.0, 0.0).astype(jnp.bfloat16)
            for step in steps
        ],
        axis=0,
    )


def slot_places(meta, me, capacity):
    count = meta.shape[1]
    turned = jnp.transpose(meta)
    relative = turned[:, 0:2].astype(jnp.int32) ^ me
    expert_at = lax.broadcasted_iota(jnp.int32, (count, 128), 1)
    row_at = lax.broadcasted_iota(jnp.int32, (count, count), 0)
    col_at = lax.broadcasted_iota(jnp.int32, (count, count), 1)
    chosen = [expert_at == relative[:, j : j + 1] for j in range(2)]
    after = jnp.where(row_at > col_at, 1.0, 0.0).astype(jnp.bfloat16)
    counted = jnp.dot(
        after,
        jnp.where(chosen[0] | chosen[1], 1.0, 0.0).astype(jnp.bfloat16),
        preferred_element_type=jnp.float32,
    )
    places = [
        relative[:, j : j + 1] * capacity
        + jnp.sum(jnp.where(chosen[j], counted, 0.0), axis=1, keepdims=True).astype(jnp.int32)
        for j in range(2)
    ]
    return places, [turned[:, 2 + j : 3 + j] for j in range(2)]


def weight_matrix(places, weights, first, amount):
    at = lax.broadcasted_iota(jnp.int32, (places[0].shape[0], amount), 1) + first
    scale = jnp.where(at == places[0], weights[0], 0.0) + jnp.where(
        at == places[1], weights[1], 0.0
    )
    upper = scale.astype(jnp.bfloat16)
    return upper, (scale - upper.astype(jnp.float32)).astype(jnp.bfloat16)


def weighted(pair, block):
    return jnp.dot(pair[0], block, preferred_element_type=jnp.float32) + jnp.dot(
        pair[1], block, preferred_element_type=jnp.float32
    )


def layer_kernel(
    peers,
    capacity,
    pieces,
    tokens,
    gain,
    meta,
    expert_gate,
    expert_up,
    expert_down,
    shared_gate,
    shared_up,
    shared_down,
    mixed,
    gate_all,
    up_all,
    down_all,
    s_gate_all,
    s_up_all,
    s_down_all,
    normed,
    cut,
    outgoing,
    received,
    results,
    returned,
    total,
    relay_in,
    meta_in,
    relay_out,
    relay_back,
    sums_out,
    sums_in,
    weight_local,
    weight_send,
    weight_recv,
    out_send,
    out_recv,
    back_send,
    back_recv,
    block_send,
    block_recv,
    meta_send,
    meta_recv,
    relay_send,
    relay_recv,
    home_send,
    home_recv,
    sums_send,
    sums_recv,
):
    me = lax.axis_index("ep")
    core = lax.axis_index("tp")
    sibling = 1 - core
    width = tokens.shape[1]
    piece = width // pieces
    half, quarter = peers // 2, peers // 4

    def is_inner(index):
        return ((index // quarter + 1) // 2) % 2

    inner = is_inner(me)
    turns = (half, half + quarter)

    def at_step(step):
        return (toggled(me, step, peers), core)

    def remote(source, target, send, recv, place):
        return pltpu.make_async_remote_copy(
            src_ref=source,
            dst_ref=target,
            send_sem=send,
            recv_sem=recv,
            device_id=place,
            device_id_type=MESH,
        )

    barrier = pltpu.get_barrier_semaphore()
    partners = list(range(1, half)) + list(turns)
    pl.semaphore_signal(barrier, inc=1, device_id=(me, sibling), device_id_type=MESH)
    for step in partners:
        pl.semaphore_signal(barrier, inc=1, device_id=at_step(step), device_id_type=MESH)
    sources = (
        (shared_gate, s_gate_all),
        (shared_up, s_up_all),
        (shared_down, s_down_all),
        (expert_gate, gate_all),
        (expert_up, up_all),
        (expert_down, down_all),
    )
    local = [
        pltpu.make_async_copy(source, target.at[core], weight_local.at[i])
        for i, (source, target) in enumerate(sources)
    ]
    for copy in local:
        copy.start()

    values = tokens[...].astype(jnp.float32)
    factor = lax.rsqrt(jnp.mean(values * values, axis=1, keepdims=True) + epsilon)
    scaled = (values * factor * gain[...]).astype(jnp.bfloat16)
    normed[...] = scaled
    for c in range(pieces):
        cut[c] = scaled[:, c * piece : (c + 1) * piece]

    gateway = at_step(half + quarter * inner)

    def block_copy(c):
        return remote(
            cut.at[c], relay_in.at[inner, c], block_send.at[c], block_recv.at[inner, c], gateway
        )

    meta_copy = remote(meta, meta_in.at[inner], meta_send.at[0], meta_recv.at[inner], gateway)

    def send_block():
        meta_copy.start()
        for c in range(pieces):
            block_copy(c).start()

    def dispatch(step):
        return remote(
            outgoing.at[step],
            received.at[step],
            out_send.at[step],
            out_recv.at[step],
            at_step(step),
        )

    def give_back(step):
        return remote(
            results.at[step],
            returned.at[step],
            back_send.at[step],
            back_recv.at[step],
            at_step(step),
        )

    pl.semaphore_wait(barrier, len(partners) + 1)

    @pl.when(inner == 1)
    def _():
        send_block()

    slots = slot_rows(meta[...], me, half)
    for first in (quarter, 0):
        rows = jnp.dot(
            picks(slots, range(first, first + quarter), capacity),
            normed[...],
            preferred_element_type=jnp.float32,
        ).astype(jnp.bfloat16)
        for i in range(quarter):
            block = rows[i * capacity : (i + 1) * capacity]
            if first + i == 0:
                received[0] = block
            else:
                outgoing[first + i] = block
                dispatch(first + i).start()

    @pl.when(inner == 0)
    def _():
        send_block()

    swaps = [
        remote(source, target.at[core], weight_send.at[i], weight_recv.at[i], (me, sibling))
        for i, (source, target) in enumerate(sources)
    ]
    for copy in swaps:
        copy.start()

    def relay(side, k, c):
        turn = turns[side]
        columns = pl.ds(c * piece, piece)
        return remote(
            relay_out.at[side, k, :, columns],
            received.at[k ^ turn, :, columns],
            relay_send.at[side * half + k, c],
            relay_recv.at[(k ^ turn) - half, c],
            at_step(k),
        )

    def pass_on(side):
        remote(
            meta, meta_in.at[side], meta_send.at[0], meta_recv.at[side], at_step(turns[side])
        ).wait_recv()
        picked = picks(slot_rows(meta_in[side], me, half), range(half), capacity)
        for c in range(pieces):
            columns = pl.ds(c * piece, piece)
            remote(
                cut.at[c],
                relay_in.at[side, c],
                block_send.at[c],
                block_recv.at[side, c],
                at_step(turns[side]),
            ).wait_recv()
            rows = jnp.dot(
                picked, relay_in[side, c], preferred_element_type=jnp.float32
            ).astype(jnp.bfloat16)
            received[turns[side], :, columns] = rows[:capacity]
            for k in range(half - 1, 0, -1):
                relay_out[side, k, :, columns] = rows[k * capacity : (k + 1) * capacity]
                relay(side, k, c).start()

    @pl.when(inner == 1)
    def _():
        pass_on(1)

    for i in range(len(sources)):
        local[i].wait()
        swaps[i].wait()

    def near(pair, carry):
        for i in range(2):
            step = 2 * pair + i

            @pl.when(step > 0)
            def _():
                dispatch(step).wait_recv()

        block = received[pl.ds(2 * pair, 2)].reshape(2 * capacity, width)
        out = gated_sum(block, gate_all, up_all, down_all).astype(jnp.bfloat16)
        for i in range(2):
            step = 2 * pair + i
            part = out[i * capacity : (i + 1) * capacity]

            @pl.when(step > 0)
            def _():
                results[step] = part
                give_back(step).start()

            @pl.when(step == 0)
            def _():
                returned[step] = part

        return carry

    total[...] = gated_sum(normed[...], s_gate_all, s_up_all, s_down_all)
    lax.fori_loop(0, half // 2, near, 0)

    @pl.when(inner == 1)
    def _():
        pass_on(0)

    def side_of(step):
        side = is_inner(toggled(me, step, peers))
        return side, toggled(step, half + quarter * side, peers)

    def home(step):
        side, k = side_of(step)
        return remote(
            results.at[step],
            relay_back.at[side, k],
            home_send.at[step - half],
            home_recv.at[side * half + k],
            at_step(k),
        )

    def far(pair, carry):
        start = half + (2 * pair + quarter * inner) % half
        for i in range(2):
            step = start + i
            side, k = side_of(step)

            @pl.when(k > 0)
            def _():
                for c in range(pieces):
                    columns = pl.ds(c * piece, piece)
                    remote(
                        relay_out.at[0, 1, :, columns],
                        received.at[step, :, columns],
                        relay_send.at[1, c],
                        relay_recv.at[step - half, c],
                        at_step(1),
                    ).wait_recv()

        block = received[pl.ds(start, 2)].reshape(2 * capacity, width)
        out = gated_sum(block, gate_all, up_all, down_all).astype(jnp.bfloat16)
        for i in range(2):
            step = start + i
            side, k = side_of(step)
            part = out[i * capacity : (i + 1) * capacity]

            @pl.when(k > 0)
            def _():
                results[step] = part
                home(step).start()

            @pl.when(k == 0)
            def _():
                relay_back[side, 0] = part

        return carry

    lax.fori_loop(0, half // 2, far, 0)

    def sums(side, c):
        return remote(
            sums_out.at[side, c],
            sums_in.at[c],
            sums_send.at[side * pieces + c],
            sums_recv.at[c],
            at_step(turns[side]),
        )

    @pl.when(inner == 1)
    def _():
        for side in (1, 0):
            places, scales = slot_places(meta_in[side], me, capacity)
            pair = weight_matrix(places, scales, 0, half * capacity)
            for k in range(1, half):
                remote(
                    results.at[half],
                    relay_back.at[side, k],
                    home_send.at[0],
                    home_recv.at[side * half + k],
                    at_step(k),
                ).wait_recv()
            for c in range(pieces):
                block = relay_back[side, :, :, pl.ds(c * piece, piece)]
                sums_out[side, c] = weighted(
                    pair, block.reshape(half * capacity, piece)
                ).astype(jnp.bfloat16)
                sums(side, c).start()

    places, scales = slot_places(meta[...], me, capacity)
    for step in range(1, half):
        give_back(step).wait_recv()
    pair = weight_matrix(places, scales, 0, half * capacity)
    total[...] += weighted(pair, returned[...].reshape(half * capacity, width))
    for c in range(pieces):
        remote(
            sums_out.at[0, c], sums_in.at[c], sums_send.at[c], sums_recv.at[c], gateway
        ).wait_recv()
        columns = pl.ds(c * piece, piece)
        mixed[:, columns] = (total[:, columns] + sums_in[c].astype(jnp.float32)).astype(
            jnp.bfloat16
        )

    for step in range(1, half):
        dispatch(step).wait_send()
        give_back(step).wait_send()
    meta_copy.wait_send()
    for c in range(pieces):
        block_copy(c).wait_send()

    def settle(i, carry):
        step = half + i
        _, k = side_of(step)

        @pl.when(k > 0)
        def _():
            home(step).wait_send()

        return carry

    lax.fori_loop(0, half, settle, 0)

    @pl.when(inner == 1)
    def _():
        for side in range(2):
            for c in range(pieces):
                sums(side, c).wait_send()
                for k in range(1, half):
                    relay(side, k, c).wait_send()


def kernel_body(
    tokens,
    norm_gain,
    expert_ids,
    route_weights,
    expert_gate,
    expert_up,
    expert_down,
    shared_gate,
    shared_up,
    shared_down,
):
    peers = lax.axis_size("ep")
    halves = lax.axis_size("tp")
    tok_rows, width = tokens.shape
    capacity = 3 * tok_rows * expert_ids.shape[1] // (2 * peers)
    half, pieces = peers // 2, 4
    vmem = pl.BlockSpec(memory_space=pltpu.VMEM)
    anywhere = pl.BlockSpec(memory_space=pl.ANY)
    weights = (
        expert_gate[0],
        expert_up[0],
        expert_down[0],
        shared_gate,
        shared_up,
        shared_down,
    )
    meta = jnp.concatenate(
        [expert_ids.astype(jnp.float32), route_weights, jnp.zeros((tok_rows, 4), jnp.float32)],
        axis=1,
    ).T

    def rows(*shape):
        return pltpu.VMEM(shape, jnp.bfloat16)

    dma = pltpu.SemaphoreType.DMA
    return pl.pallas_call(
        functools.partial(layer_kernel, peers, capacity, pieces),
        out_shape=jax.ShapeDtypeStruct((tok_rows, width), jnp.bfloat16),
        in_specs=[vmem] * 3 + [anywhere] * 6,
        out_specs=vmem,
        scratch_shapes=[pltpu.VMEM((halves,) + w.shape, w.dtype) for w in weights]
        + [
            rows(tok_rows, width),
            rows(pieces, tok_rows, width // pieces),
            rows(half, capacity, width),
            rows(peers, capacity, width),
            rows(peers, capacity, width),
            rows(half, capacity, width),
            pltpu.VMEM((tok_rows, width), jnp.float32),
            rows(2, pieces, tok_rows, width // pieces),
            pltpu.VMEM((2,) + meta.shape, jnp.float32),
            rows(2, half, capacity, width),
            rows(2, half, capacity, width),
            rows(2, pieces, tok_rows, width // pieces),
            rows(pieces, tok_rows, width // pieces),
        ]
        + [dma((len(weights),))] * 3
        + [dma((half,))] * 4
        + [dma((pieces,)), dma((2, pieces)), dma((1,)), dma((2,))]
        + [dma((2 * half, pieces)), dma((half, pieces))]
        + [dma((half,)), dma((2 * half,))]
        + [dma((2 * pieces,)), dma((pieces,))],
        compiler_params=pltpu.CompilerParams(
            collective_id=0, has_side_effects=True, vmem_limit_bytes=60 * 1024 * 1024
        ),
        name="layer",
    )(tokens, norm_gain.reshape(1, width), meta, *weights)


def normalize(tokens, norm_gain):
    values = tokens.astype(jnp.float32)
    factor = lax.rsqrt(jnp.mean(values * values, axis=1, keepdims=True) + epsilon)
    return (values * factor * norm_gain[None, :]).astype(jnp.bfloat16)


def round_term(partial_value):
    return lax.optimization_barrier(partial_value.astype(jnp.bfloat16)).astype(jnp.float32)


def gated_rows(row_block, gate_w, up_w):
    gate_value = jnp.dot(row_block, gate_w, preferred_element_type=jnp.float32)
    up_value = jnp.dot(row_block, up_w, preferred_element_type=jnp.float32)
    return (jax.nn.silu(gate_value) * up_value).astype(jnp.bfloat16)


def sliced_term(hidden, down_w):
    return round_term(jnp.dot(hidden, down_w, preferred_element_type=jnp.float32))


def shared_branch(normed, shared_gate, shared_up, shared_down):
    hidden = gated_rows(lax.all_gather(normed, "tp", axis=0, tiled=True), shared_gate, shared_up)
    return lax.psum_scatter(
        sliced_term(hidden, shared_down).astype(jnp.bfloat16), "tp", scatter_dimension=0, tiled=True
    ).astype(jnp.float32)


def body(
    tokens,
    norm_gain,
    expert_ids,
    route_weights,
    expert_gate,
    expert_up,
    expert_down,
    shared_gate,
    shared_up,
    shared_down,
):
    normed = normalize(tokens, norm_gain)
    tok_rows = tokens.shape[0]
    model_width = tokens.shape[1]
    top_count = expert_ids.shape[1]
    ep_size = lax.axis_size("ep")
    experts = expert_gate.shape[0] * ep_size
    capacity = 3 * tok_rows * top_count // (2 * experts)
    assigned = tok_rows * top_count
    gate_one = expert_gate[0]
    up_one = expert_up[0]
    down_one = expert_down[0]
    flat_ids = expert_ids.reshape(-1)
    onehot = (flat_ids[:, None] == jnp.arange(experts, dtype=jnp.int32)[None, :]).astype(
        jnp.bfloat16
    )
    earlier = (jnp.arange(assigned)[:, None] > jnp.arange(assigned)[None, :]).astype(jnp.bfloat16)
    before_count = jnp.dot(earlier, onehot, preferred_element_type=jnp.float32)
    slot_index = jnp.sum(before_count * onehot.astype(jnp.float32), axis=1).astype(jnp.int32)
    position = flat_ids * capacity + slot_index
    owners = (
        jnp.full((experts * capacity,), tok_rows, jnp.int32)
        .at[position]
        .set(jnp.arange(assigned, dtype=jnp.int32) // top_count)
    )
    padded = jnp.concatenate([normed, jnp.zeros((1, model_width), jnp.bfloat16)], axis=0)
    outgoing = padded[owners].reshape(ep_size, capacity, model_width)
    half_slots = capacity // 2
    split_rows = outgoing.reshape(ep_size, 2, half_slots, model_width)
    results = []
    for portion in range(2):
        received = lax.all_to_all(
            split_rows[:, portion], "ep", split_axis=0, concat_axis=0, tiled=True
        )
        hidden = gated_rows(
            lax.all_gather(
                received.reshape(ep_size * half_slots, model_width), "tp", axis=0, tiled=True
            ),
            gate_one,
            up_one,
        )
        summed = lax.psum_scatter(
            sliced_term(hidden, down_one).astype(jnp.bfloat16),
            "tp",
            scatter_dimension=0,
            tiled=True,
        )
        results.append(
            lax.all_to_all(
                summed.reshape(ep_size, half_slots, model_width),
                "ep",
                split_axis=0,
                concat_axis=0,
                tiled=True,
            )
        )
    returned = jnp.stack(results, axis=1)
    gathered = returned.reshape(experts * capacity, model_width)[position]
    routed = jnp.sum(
        gathered.reshape(tok_rows, top_count, model_width).astype(jnp.float32)
        * route_weights[:, :, None],
        axis=1,
    )
    shared_out = shared_branch(normed, shared_gate, shared_up, shared_down)
    return (routed + shared_out).astype(jnp.bfloat16)


def plan_of(*args):
    peers = lax.axis_size("ep")
    capacity = 3 * args[0].shape[0] * args[2].shape[1] // (2 * peers)
    whole_tiles = capacity % 16 == 0 and peers % 4 == 0 and peers & (peers - 1) == 0
    fits = whole_tiles and lax.axis_size("tp") == 2 and args[4].shape[0] == 1
    return (kernel_body if fits else body)(*args)


def solution(mesh):
    placed = (
        P(("ep", "tp"), None),
        P(),
        P(("ep", "tp"), None),
        P(("ep", "tp"), None),
        P("ep", None, "tp"),
        P("ep", None, "tp"),
        P("ep", "tp", None),
        P(None, "tp"),
        P(None, "tp"),
        P("tp", None),
    )
    return jax.shard_map(
        plan_of, mesh=mesh, in_specs=placed, out_specs=P(("ep", "tp"), None), check_vma=False
    )
```

```python
import functools

import jax
import jax.numpy as jnp
from jax import lax
from jax.experimental import pallas as pl
from jax.experimental.pallas import tpu as pltpu
from jax.sharding import PartitionSpec as P

epsilon = 1e-06
MESH = pl.DeviceIdType.MESH


def toggled(index, step, size):
    total, bit = 0, 1
    while bit < size:
        total = total + bit * ((index // bit + step // bit) % 2)
        bit *= 2
    return total


def gated_sum(rows, gate_w, up_w, down_w):
    total = None
    for half in range(gate_w.shape[0]):
        gate_value = jnp.dot(rows, gate_w[half], preferred_element_type=jnp.float32)
        up_value = jnp.dot(rows, up_w[half], preferred_element_type=jnp.float32)
        hidden = (gate_value / (1.0 + jnp.exp(-gate_value)) * up_value).astype(jnp.bfloat16)
        term = jnp.dot(hidden, down_w[half], preferred_element_type=jnp.float32)
        total = term if total is None else total + term
    return total


def slot_rows(meta, me, steps):
    count = meta.shape[1]
    relative = meta[0:2, :].astype(jnp.int32) ^ me
    step_of = lax.broadcasted_iota(jnp.int32, (steps, count), 0)
    named = (step_of == relative[0:1, :]) | (step_of == relative[1:2, :])
    row_at = lax.broadcasted_iota(jnp.int32, (count, count), 0)
    col_at = lax.broadcasted_iota(jnp.int32, (count, count), 1)
    before = jnp.where(row_at < col_at, 1.0, 0.0).astype(jnp.bfloat16)
    slots = jnp.dot(
        jnp.where(named, 1.0, 0.0).astype(jnp.bfloat16), before, preferred_element_type=jnp.float32
    ).astype(jnp.int32)
    return jnp.where(named, slots, -1)


def picks(slots, steps, capacity):
    slot_at = lax.broadcasted_iota(jnp.int32, (capacity, slots.shape[1]), 0)
    return jnp.concatenate(
        [
            jnp.where(slot_at == slots[step : step + 1, :], 1.0, 0.0).astype(jnp.bfloat16)
            for step in steps
        ],
        axis=0,
    )


def slot_places(meta, me, capacity):
    count = meta.shape[1]
    turned = jnp.transpose(meta)
    relative = turned[:, 0:2].astype(jnp.int32) ^ me
    expert_at = lax.broadcasted_iota(jnp.int32, (count, 128), 1)
    row_at = lax.broadcasted_iota(jnp.int32, (count, count), 0)
    col_at = lax.broadcasted_iota(jnp.int32, (count, count), 1)
    chosen = [expert_at == relative[:, j : j + 1] for j in range(2)]
    after = jnp.where(row_at > col_at, 1.0, 0.0).astype(jnp.bfloat16)
    counted = jnp.dot(
        after,
        jnp.where(chosen[0] | chosen[1], 1.0, 0.0).astype(jnp.bfloat16),
        preferred_element_type=jnp.float32,
    )
    places = [
        relative[:, j : j + 1] * capacity
        + jnp.sum(jnp.where(chosen[j], counted, 0.0), axis=1, keepdims=True).astype(jnp.int32)
        for j in range(2)
    ]
    return places, [turned[:, 2 + j : 3 + j] for j in range(2)]


def weight_matrix(places, weights, first, amount):
    at = lax.broadcasted_iota(jnp.int32, (places[0].shape[0], amount), 1) + first
    scale = jnp.where(at == places[0], weights[0], 0.0) + jnp.where(
        at == places[1], weights[1], 0.0
    )
    upper = scale.astype(jnp.bfloat16)
    return upper, (scale - upper.astype(jnp.float32)).astype(jnp.bfloat16)


def weighted(pair, block):
    return jnp.dot(pair[0], block, preferred_element_type=jnp.float32) + jnp.dot(
        pair[1], block, preferred_element_type=jnp.float32
    )


def layer_kernel(
    peers,
    capacity,
    pieces,
    tokens,
    gain,
    meta,
    expert_gate,
    expert_up,
    expert_down,
    shared_gate,
    shared_up,
    shared_down,
    mixed,
    gate_all,
    up_all,
    down_all,
    s_gate_all,
    s_up_all,
    s_down_all,
    normed,
    cut,
    outgoing,
    received,
    results,
    returned,
    total,
    relay_in,
    meta_in,
    relay_out,
    relay_back,
    sums_out,
    sums_in,
    weight_local,
    weight_send,
    weight_recv,
    out_send,
    out_recv,
    back_send,
    back_recv,
    block_send,
    block_recv,
    meta_send,
    meta_recv,
    relay_send,
    relay_recv,
    home_send,
    home_recv,
    sums_send,
    sums_recv,
):
    me = lax.axis_index("ep")
    core = lax.axis_index("tp")
    sibling = 1 - core
    width = tokens.shape[1]
    piece = width // pieces
    half, quarter = peers // 2, peers // 4

    def is_inner(index):
        return ((index // quarter + 1) // 2) % 2

    inner = is_inner(me)
    turns = (half, half + quarter)

    def at_step(step):
        return (toggled(me, step, peers), core)

    def remote(source, target, send, recv, place):
        return pltpu.make_async_remote_copy(
            src_ref=source,
            dst_ref=target,
            send_sem=send,
            recv_sem=recv,
            device_id=place,
            device_id_type=MESH,
        )

    barrier = pltpu.get_barrier_semaphore()
    partners = range(1, peers)
    pl.semaphore_signal(barrier, inc=1, device_id=(me, sibling), device_id_type=MESH)
    for step in partners:
        pl.semaphore_signal(barrier, inc=1, device_id=at_step(step), device_id_type=MESH)
    sources = (
        (shared_gate, s_gate_all),
        (shared_up, s_up_all),
        (shared_down, s_down_all),
        (expert_gate, gate_all),
        (expert_up, up_all),
        (expert_down, down_all),
    )
    local = [
        pltpu.make_async_copy(source, target.at[core], weight_local.at[i])
        for i, (source, target) in enumerate(sources)
    ]
    for copy in local:
        copy.start()

    values = tokens[...].astype(jnp.float32)
    factor = lax.rsqrt(jnp.mean(values * values, axis=1, keepdims=True) + epsilon)
    scaled = (values * factor * gain[...]).astype(jnp.bfloat16)
    normed[...] = scaled
    for c in range(pieces):
        cut[c] = scaled[:, c * piece : (c + 1) * piece]

    gateway = at_step(half + quarter * inner)

    def block_copy(c):
        return remote(
            cut.at[c], relay_in.at[inner, c], block_send.at[c], block_recv.at[inner, c], gateway
        )

    meta_copy = remote(meta, meta_in.at[inner], meta_send.at[0], meta_recv.at[inner], gateway)

    def send_block():
        meta_copy.start()
        for c in range(pieces):
            block_copy(c).start()

    def dispatch(step):
        return remote(
            outgoing.at[step],
            received.at[step],
            out_send.at[step],
            out_recv.at[step],
            at_step(step),
        )

    def give_back(step):
        return remote(
            results.at[step],
            returned.at[step],
            back_send.at[step],
            back_recv.at[step],
            at_step(step),
        )

    pl.semaphore_wait(barrier, len(partners) + 1)

    @pl.when(inner == 1)
    def _():
        send_block()

    slots = slot_rows(meta[...], me, peers)

    def send_slots(first):
        rows = jnp.dot(
            picks(slots, range(first, first + quarter), capacity),
            normed[...],
            preferred_element_type=jnp.float32,
        ).astype(jnp.bfloat16)
        for i in range(quarter):
            block = rows[i * capacity : (i + 1) * capacity]
            if first + i == 0:
                received[0] = block
            else:
                outgoing[first + i] = block
                dispatch(first + i).start()

    send_slots(quarter)
    send_slots(0)

    @pl.when(inner == 0)
    def _():
        send_slots(half + quarter)
        send_slots(half)

    swaps = [
        remote(source, target.at[core], weight_send.at[i], weight_recv.at[i], (me, sibling))
        for i, (source, target) in enumerate(sources)
    ]
    for copy in swaps:
        copy.start()

    def relay(side, k, c):
        turn = turns[side]
        columns = pl.ds(c * piece, piece)
        return remote(
            relay_out.at[side, k, :, columns],
            received.at[k ^ turn, :, columns],
            relay_send.at[side * half + k, c],
            relay_recv.at[(k ^ turn) - half, c],
            at_step(k),
        )

    def pass_on(side):
        remote(
            meta, meta_in.at[side], meta_send.at[0], meta_recv.at[side], at_step(turns[side])
        ).wait_recv()
        picked = picks(slot_rows(meta_in[side], me, half), range(half), capacity)
        for c in range(pieces):
            columns = pl.ds(c * piece, piece)
            remote(
                cut.at[c],
                relay_in.at[side, c],
                block_send.at[c],
                block_recv.at[side, c],
                at_step(turns[side]),
            ).wait_recv()
            rows = jnp.dot(
                picked, relay_in[side, c], preferred_element_type=jnp.float32
            ).astype(jnp.bfloat16)
            received[turns[side], :, columns] = rows[:capacity]
            for k in range(half - 1, 0, -1):
                relay_out[side, k, :, columns] = rows[k * capacity : (k + 1) * capacity]
                relay(side, k, c).start()

    @pl.when(inner == 1)
    def _():
        pass_on(1)

    for i in range(len(sources)):
        local[i].wait()
        swaps[i].wait()

    def near(pair, carry):
        for i in range(2):
            step = 2 * pair + i

            @pl.when(step > 0)
            def _():
                dispatch(step).wait_recv()

        block = received[pl.ds(2 * pair, 2)].reshape(2 * capacity, width)
        out = gated_sum(block, gate_all, up_all, down_all).astype(jnp.bfloat16)
        for i in range(2):
            step = 2 * pair + i
            part = out[i * capacity : (i + 1) * capacity]

            @pl.when(step > 0)
            def _():
                results[step] = part
                give_back(step).start()

            @pl.when(step == 0)
            def _():
                returned[step] = part

        return carry

    total[...] = gated_sum(normed[...], s_gate_all, s_up_all, s_down_all)
    lax.fori_loop(0, half // 2, near, 0)

    def side_of(step):
        side = is_inner(toggled(me, step, peers))
        return side, toggled(step, half + quarter * side, peers)

    def home(step):
        side, k = side_of(step)
        return remote(
            results.at[step],
            relay_back.at[side, k],
            home_send.at[step - half],
            home_recv.at[side * half + k],
            at_step(k),
        )

    def far(pair, carry):
        start = half + (2 * pair + quarter * inner) % half
        for i in range(2):
            step = start + i
            side, k = side_of(step)

            @pl.when(side == 0)
            def _():
                dispatch(step).wait_recv()

            @pl.when((side == 1) & (k > 0))
            def _():
                for c in range(pieces):
                    columns = pl.ds(c * piece, piece)
                    remote(
                        relay_out.at[0, 1, :, columns],
                        received.at[step, :, columns],
                        relay_send.at[1, c],
                        relay_recv.at[step - half, c],
                        at_step(1),
                    ).wait_recv()

        block = received[pl.ds(start, 2)].reshape(2 * capacity, width)
        out = gated_sum(block, gate_all, up_all, down_all).astype(jnp.bfloat16)
        for i in range(2):
            step = start + i
            side, k = side_of(step)
            part = out[i * capacity : (i + 1) * capacity]

            @pl.when(side == 0)
            def _():
                results[step] = part
                give_back(step).start()

            @pl.when((side == 1) & (k > 0))
            def _():
                results[step] = part
                home(step).start()

            @pl.when((side == 1) & (k == 0))
            def _():
                relay_back[1, 0] = part

        return carry

    lax.fori_loop(0, half // 2, far, 0)

    def sums(side, c):
        return remote(
            sums_out.at[side, c],
            sums_in.at[c],
            sums_send.at[side * pieces + c],
            sums_recv.at[c],
            at_step(turns[side]),
        )

    @pl.when(inner == 1)
    def _():
        for side in (1,):
            places, scales = slot_places(meta_in[side], me, capacity)
            pair = weight_matrix(places, scales, 0, half * capacity)
            for k in range(1, half):
                remote(
                    results.at[half],
                    relay_back.at[side, k],
                    home_send.at[0],
                    home_recv.at[side * half + k],
                    at_step(k),
                ).wait_recv()
            for c in range(pieces):
                block = relay_back[side, :, :, pl.ds(c * piece, piece)]
                sums_out[side, c] = weighted(
                    pair, block.reshape(half * capacity, piece)
                ).astype(jnp.bfloat16)
                sums(side, c).start()

    places, scales = slot_places(meta[...], me, capacity)
    for step in range(1, half):
        give_back(step).wait_recv()
    pair = weight_matrix(places, scales, 0, half * capacity)
    total[...] += weighted(pair, returned[:half].reshape(half * capacity, width))

    @pl.when(inner == 1)
    def _():
        for c in range(pieces):
            sums(1, c).wait_recv()
            columns = pl.ds(c * piece, piece)
            mixed[:, columns] = (total[:, columns] + sums_in[c].astype(jnp.float32)).astype(
                jnp.bfloat16
            )

    @pl.when(inner == 0)
    def _():
        for first in (half, half + quarter):
            for i in range(quarter):
                give_back(first + i).wait_recv()
            pair = weight_matrix(places, scales, first * capacity, quarter * capacity)
            block = returned[first : first + quarter].reshape(quarter * capacity, width)
            term = total[...] + weighted(pair, block)
            if first == half:
                total[...] = term
            else:
                mixed[...] = term.astype(jnp.bfloat16)
        for step in range(half, peers):
            dispatch(step).wait_send()

    for step in range(1, half):
        dispatch(step).wait_send()
        give_back(step).wait_send()

    def settle(i, carry):
        step = half + i
        side, k = side_of(step)

        @pl.when(side == 0)
        def _():
            give_back(step).wait_send()

        @pl.when((side == 1) & (k > 0))
        def _():
            home(step).wait_send()

        return carry

    lax.fori_loop(0, half, settle, 0)

    @pl.when(inner == 1)
    def _():
        meta_copy.wait_send()
        for side in (1,):
            for c in range(pieces):
                block_copy(c).wait_send()
                sums(side, c).wait_send()
                for k in range(1, half):
                    relay(side, k, c).wait_send()


def kernel_body(
    tokens,
    norm_gain,
    expert_ids,
    route_weights,
    expert_gate,
    expert_up,
    expert_down,
    shared_gate,
    shared_up,
    shared_down,
):
    peers = lax.axis_size("ep")
    halves = lax.axis_size("tp")
    tok_rows, width = tokens.shape
    capacity = 3 * tok_rows * expert_ids.shape[1] // (2 * peers)
    half, pieces = peers // 2, 4
    vmem = pl.BlockSpec(memory_space=pltpu.VMEM)
    anywhere = pl.BlockSpec(memory_space=pl.ANY)
    weights = (
        expert_gate[0],
        expert_up[0],
        expert_down[0],
        shared_gate,
        shared_up,
        shared_down,
    )
    meta = jnp.concatenate(
        [expert_ids.astype(jnp.float32), route_weights, jnp.zeros((tok_rows, 4), jnp.float32)],
        axis=1,
    ).T

    def rows(*shape):
        return pltpu.VMEM(shape, jnp.bfloat16)

    dma = pltpu.SemaphoreType.DMA
    return pl.pallas_call(
        functools.partial(layer_kernel, peers, capacity, pieces),
        out_shape=jax.ShapeDtypeStruct((tok_rows, width), jnp.bfloat16),
        in_specs=[vmem] * 3 + [anywhere] * 6,
        out_specs=vmem,
        scratch_shapes=[pltpu.VMEM((halves,) + w.shape, w.dtype) for w in weights]
        + [
            rows(tok_rows, width),
            rows(pieces, tok_rows, width // pieces),
            rows(peers, capacity, width),
            rows(peers, capacity, width),
            rows(peers, capacity, width),
            rows(peers, capacity, width),
            pltpu.VMEM((tok_rows, width), jnp.float32),
            rows(2, pieces, tok_rows, width // pieces),
            pltpu.VMEM((2,) + meta.shape, jnp.float32),
            rows(2, half, capacity, width),
            rows(2, half, capacity, width),
            rows(2, pieces, tok_rows, width // pieces),
            rows(pieces, tok_rows, width // pieces),
        ]
        + [dma((len(weights),))] * 3
        + [dma((peers,))] * 4
        + [dma((pieces,)), dma((2, pieces)), dma((1,)), dma((2,))]
        + [dma((2 * half, pieces)), dma((half, pieces))]
        + [dma((half,)), dma((2 * half,))]
        + [dma((2 * pieces,)), dma((pieces,))],
        compiler_params=pltpu.CompilerParams(
            collective_id=0, has_side_effects=True, vmem_limit_bytes=60 * 1024 * 1024
        ),
        name="layer",
    )(tokens, norm_gain.reshape(1, width), meta, *weights)


def normalize(tokens, norm_gain):
    values = tokens.astype(jnp.float32)
    factor = lax.rsqrt(jnp.mean(values * values, axis=1, keepdims=True) + epsilon)
    return (values * factor * norm_gain[None, :]).astype(jnp.bfloat16)


def round_term(partial_value):
    return lax.optimization_barrier(partial_value.astype(jnp.bfloat16)).astype(jnp.float32)


def gated_rows(row_block, gate_w, up_w):
    gate_value = jnp.dot(row_block, gate_w, preferred_element_type=jnp.float32)
    up_value = jnp.dot(row_block, up_w, preferred_element_type=jnp.float32)
    return (jax.nn.silu(gate_value) * up_value).astype(jnp.bfloat16)


def sliced_term(hidden, down_w):
    return round_term(jnp.dot(hidden, down_w, preferred_element_type=jnp.float32))


def shared_branch(normed, shared_gate, shared_up, shared_down):
    hidden = gated_rows(lax.all_gather(normed, "tp", axis=0, tiled=True), shared_gate, shared_up)
    return lax.psum_scatter(
        sliced_term(hidden, shared_down).astype(jnp.bfloat16), "tp", scatter_dimension=0, tiled=True
    ).astype(jnp.float32)


def body(
    tokens,
    norm_gain,
    expert_ids,
    route_weights,
    expert_gate,
    expert_up,
    expert_down,
    shared_gate,
    shared_up,
    shared_down,
):
    normed = normalize(tokens, norm_gain)
    tok_rows = tokens.shape[0]
    model_width = tokens.shape[1]
    top_count = expert_ids.shape[1]
    ep_size = lax.axis_size("ep")
    experts = expert_gate.shape[0] * ep_size
    capacity = 3 * tok_rows * top_count // (2 * experts)
    assigned = tok_rows * top_count
    gate_one = expert_gate[0]
    up_one = expert_up[0]
    down_one = expert_down[0]
    flat_ids = expert_ids.reshape(-1)
    onehot = (flat_ids[:, None] == jnp.arange(experts, dtype=jnp.int32)[None, :]).astype(
        jnp.bfloat16
    )
    earlier = (jnp.arange(assigned)[:, None] > jnp.arange(assigned)[None, :]).astype(jnp.bfloat16)
    before_count = jnp.dot(earlier, onehot, preferred_element_type=jnp.float32)
    slot_index = jnp.sum(before_count * onehot.astype(jnp.float32), axis=1).astype(jnp.int32)
    position = flat_ids * capacity + slot_index
    owners = (
        jnp.full((experts * capacity,), tok_rows, jnp.int32)
        .at[position]
        .set(jnp.arange(assigned, dtype=jnp.int32) // top_count)
    )
    padded = jnp.concatenate([normed, jnp.zeros((1, model_width), jnp.bfloat16)], axis=0)
    outgoing = padded[owners].reshape(ep_size, capacity, model_width)
    half_slots = capacity // 2
    split_rows = outgoing.reshape(ep_size, 2, half_slots, model_width)
    results = []
    for portion in range(2):
        received = lax.all_to_all(
            split_rows[:, portion], "ep", split_axis=0, concat_axis=0, tiled=True
        )
        hidden = gated_rows(
            lax.all_gather(
                received.reshape(ep_size * half_slots, model_width), "tp", axis=0, tiled=True
            ),
            gate_one,
            up_one,
        )
        summed = lax.psum_scatter(
            sliced_term(hidden, down_one).astype(jnp.bfloat16),
            "tp",
            scatter_dimension=0,
            tiled=True,
        )
        results.append(
            lax.all_to_all(
                summed.reshape(ep_size, half_slots, model_width),
                "ep",
                split_axis=0,
                concat_axis=0,
                tiled=True,
            )
        )
    returned = jnp.stack(results, axis=1)
    gathered = returned.reshape(experts * capacity, model_width)[position]
    routed = jnp.sum(
        gathered.reshape(tok_rows, top_count, model_width).astype(jnp.float32)
        * route_weights[:, :, None],
        axis=1,
    )
    shared_out = shared_branch(normed, shared_gate, shared_up, shared_down)
    return (routed + shared_out).astype(jnp.bfloat16)


def plan_of(*args):
    peers = lax.axis_size("ep")
    capacity = 3 * args[0].shape[0] * args[2].shape[1] // (2 * peers)
    whole_tiles = capacity % 16 == 0 and peers % 4 == 0 and peers & (peers - 1) == 0
    fits = whole_tiles and lax.axis_size("tp") == 2 and args[4].shape[0] == 1
    return (kernel_body if fits else body)(*args)


def solution(mesh):
    placed = (
        P(("ep", "tp"), None),
        P(),
        P(("ep", "tp"), None),
        P(("ep", "tp"), None),
        P("ep", None, "tp"),
        P("ep", None, "tp"),
        P("ep", "tp", None),
        P(None, "tp"),
        P(None, "tp"),
        P("tp", None),
    )
    return jax.shard_map(
        plan_of, mesh=mesh, in_specs=placed, out_specs=P(("ep", "tp"), None), check_vma=False
    )
```
